32 devices in a mesh: grp: 2 (over x), ep: 8 (over z, y), tp: 2 (over core).
Axes of the slice: x: 2, y: 2, z: 4, core: 2. Of those that a mesh axis runs over, the one named last changes fastest.
Arguments:
- tokens: bfloat16 [1024, 2048], P(('grp', 'ep')), parts along dimension 0, may hold values from -6 to 6
- norm_gain: float32 [2048], replicated, may hold values from 0.1 to 1.9
- groups: int32 [1024], P(('grp', 'ep')), parts along dimension 0, may hold values from 0 to 1, as said below
- picks: int32 [1024, 4], P(('grp', 'ep')), parts along dimension 0, may hold values from 0 to 7, as said below
- gates: float32 [1024, 4], P(('grp', 'ep')), parts along dimension 0, may hold values from 0.1 to 1
- w_gate: bfloat16 [16, 2048, 512], P('ep', None, 'tp'), may hold values from -0.125 to 0.125
- w_up: bfloat16 [16, 2048, 512], P('ep', None, 'tp'), may hold values from -0.125 to 0.125
- w_down: bfloat16 [16, 512, 2048], P('ep', 'tp'), may hold values from -0.25 to 0.25
Outputs:
- mixed: bfloat16 [1024, 2048], P(('grp', 'ep'), 'tp'), parts along dimension 0
The draws below stay inside these ranges and needn't reach their ends.
There are 2 independent parts, one for each index of `grp`. The reference program is written for one: setup_inputs(seed, part) draws one part's arguments, and reference() takes and returns one part's arrays. A program takes and returns all parts, laid end to end along the dimension named above; an argument that names none is the same for every part. Nothing has to cross between parts.
Inputs may be any that keep to these rules, and one draw needn't show every extreme that they name: `groups`: among the tokens of one device, exactly 32 lie in one common group and all of them name one common expert of it as their first pick; every other token of that device lies in another group. A token's 4 picks are distinct. Among the tokens of one device at most 32 name any one expert (group and pick together), and in every draw one expert is named by exactly 32 tokens of every device.
All inputs are finite; a program needn't handle non-finite values.
Results may differ from the reference program's by a relative error of at most 0.014.
Values may be sent and summed in bfloat16 or wider, within the bound.
No kernel may reach another device: no remote copies, remote signals or barrier semaphores. Data moves between devices by JAX's collectives and lax.ppermute only.
A program may use at most 64 MiB of HBM per device.

```python
import math
import jax
import jax.numpy as jnp
from jax import lax

D = 2048
FFE = 512
GROUPS = 2
TOP_K = 4
TOK_DEV = 64
EXPERTS = 16
GROUP_EXPERTS = 8
CAP = 32
TOKENS = 512
N_EP = 8
N_TP = 2


def routing_tables(key):
    base = jax.random.fold_in(key, 7)
    keys = jax.random.split(base, 3)
    hot_group = jax.random.randint(keys[0], (), 0, GROUPS)
    hot_expert = jax.random.randint(keys[1], (), 0, GROUP_EXPERTS)
    slot = jnp.arange(TOP_K, dtype=jnp.int32)

    def one_block(block_key):
        key_perm, key_hot, key_rest, key_group = jax.random.split(block_key, 4)
        order = jax.random.permutation(key_perm, TOK_DEV).astype(jnp.int32)
        offset_hot = jax.random.randint(key_hot, (), 0, GROUP_EXPERTS - 1)
        offset_rest = jax.random.randint(key_rest, (), 0, GROUP_EXPERTS)
        other = (hot_group + 1 + jax.random.randint(key_group, (TOK_DEV,), 0, GROUPS - 1)) % GROUPS
        is_hot = order < CAP
        step_hot = order[:, None] * (TOP_K - 1) + slot[None, :] - 1
        hot_values = jnp.where(slot[None, :] == 0, hot_expert, (hot_expert + 1 + (offset_hot + step_hot) % (GROUP_EXPERTS - 1)) % GROUP_EXPERTS)
        step_rest = (order[:, None] - CAP) * TOP_K + slot[None, :]
        rest_values = (offset_rest + step_rest) % GROUP_EXPERTS
        chosen = jnp.where(is_hot[:, None], hot_values, rest_values)
        group_of = jnp.where(is_hot, hot_group, other)
        return (group_of.astype(jnp.int32), chosen.astype(jnp.int32))
    block_keys = jax.random.split(keys[2], TOKENS // TOK_DEV)
    group_of, chosen = jax.vmap(one_block)(block_keys)
    return (group_of.reshape(TOKENS), chosen.reshape(TOKENS, TOP_K))


def draw_groups(key, part):
    return routing_tables(key)[0]


def draw_picks(key, part):
    return routing_tables(key)[1]


def block_scale(rng, shape, cuts, low, high):
    factor_of, own = 1.0, jax.random.fold_in(rng, 6)
    for dim, blocks in cuts:
        steps = jnp.exp(jax.random.uniform(jax.random.fold_in(own, dim), (blocks,), jnp.float32, low / len(cuts), high / len(cuts)))
        factor_of = factor_of * jnp.repeat(steps, shape[dim] // blocks).reshape([-1 if axis == dim else 1 for axis in range(len(shape))])
    return factor_of


def bell_draw(own_key, dims, scale, bound, shards=(), kind=jnp.bfloat16):
    result = scale * jax.random.normal(own_key, dims, jnp.float32)
    if shards:
        result = result * block_scale(own_key, dims, shards, -0.22, 0.18)
    return jnp.clip(result, -bound, bound).astype(kind)


def setup_inputs(seed: int = 0, part: int = 0) -> dict:
    key_list = jax.random.split(jax.random.key(seed), 9)
    own_keys = jax.random.split(jax.random.fold_in(key_list[8], part), 9)
    tokens = bell_draw(own_keys[0], (TOKENS, D), 1.0, 6.0, ((0, 8),))
    norm_gain = jnp.clip(1.0 + 0.18 * jax.random.normal(key_list[1], (D,), jnp.float32), 0.1, 1.9)
    groups = draw_groups(jax.random.fold_in(jax.random.fold_in(key_list[8], part), 71), part)
    picks = draw_picks(jax.random.fold_in(jax.random.fold_in(key_list[8], part), 71), part)
    gates = jnp.clip(jnp.exp(math.log(1.0) - 2.3025851 * jax.random.uniform(own_keys[4], (TOKENS, TOP_K), jnp.float32) ** block_scale(own_keys[4], (TOKENS, TOP_K), ((0, 8),), -0.2, 0.2)), 0.1, 1.0)
    w_gate = bell_draw(key_list[5], (EXPERTS, D, FFE), D ** -0.5, 0.125, ((0, 8), (2, 2)))
    w_up = bell_draw(key_list[6], (EXPERTS, D, FFE), D ** -0.5, 0.125, ((0, 8), (2, 2)))
    w_down = bell_draw(key_list[7], (EXPERTS, FFE, D), FFE ** -0.5, 0.25, ((0, 8), (1, 2)))
    return dict(tokens=tokens, norm_gain=norm_gain, groups=groups, picks=picks, gates=gates, w_gate=w_gate, w_up=w_up, w_down=w_down)


epsilon = 1e-06

def reference(tokens, norm_gain, groups, picks, gates, w_gate, w_up, w_down):
    values = tokens.astype(jnp.float32)
    normed = (values * lax.rsqrt(lax.optimization_barrier(jnp.mean(values * values, axis=-1, keepdims=True)) + epsilon) * norm_gain.astype(jnp.float32)).astype(jnp.bfloat16)
    expert_id = groups[:, None] * GROUP_EXPERTS + picks
    limit = N_EP * CAP
    slots = jnp.arange(limit, dtype=jnp.int32)

    def per_expert(total, inputs):
        expert, wg, wu, wd = inputs
        hit = expert_id == expert
        gate_me = lax.optimization_barrier(jnp.sum(jnp.where(hit, gates, 0.0), axis=1))
        present = jnp.any(hit, axis=1)
        position = jnp.cumsum(present.astype(jnp.int32)) - 1
        select = jnp.logical_and(position[None, :] == slots[:, None], present[None, :]).astype(jnp.float32)
        rows = jnp.dot(select.astype(jnp.bfloat16), normed, preferred_element_type=jnp.float32).astype(jnp.bfloat16)
        gate_pre = jnp.dot(rows, wg, preferred_element_type=jnp.float32)
        up_pre = jnp.dot(rows, wu, preferred_element_type=jnp.float32)
        hidden = (jax.nn.silu(gate_pre) * up_pre).astype(jnp.bfloat16)
        blocks = hidden.reshape(limit, N_TP, FFE // N_TP).astype(jnp.float32)
        down = wd.reshape(N_TP, FFE // N_TP, D).astype(jnp.float32)
        parts = jnp.einsum('rkf,kfd->krd', blocks, down).astype(jnp.bfloat16)
        expert_out = lax.optimization_barrier(jnp.sum(parts.astype(jnp.float32), axis=0)).astype(jnp.bfloat16)
        weighted = (select * gate_me[None, :]).T
        return (total + jnp.dot(weighted, expert_out.astype(jnp.float32), precision=lax.Precision.HIGHEST), None)
    start = jnp.zeros((tokens.shape[0], D), jnp.float32)
    total, unused = lax.scan(per_expert, start, (jnp.arange(EXPERTS, dtype=jnp.int32), w_gate, w_up, w_down))
    return total.astype(jnp.bfloat16)
```

```python
import jax
import jax.numpy as jnp
from jax import lax
from jax.sharding import PartitionSpec as P

GROUPS = 2
LANES = 128

epsilon = 1e-06


def on_device(tokens, norm_gain, groups, picks, gates, w_gate, w_up, w_down):
    tok_rows, width = tokens.shape
    top = picks.shape[1]
    local = w_gate.shape[0]
    senders = lax.axis_size("ep")
    cores = lax.axis_size("tp")
    group_experts = senders * local // GROUPS
    capacity = tok_rows * top // group_experts
    rows = max(capacity, tok_rows - capacity)
    team = senders // GROUPS
    half = width // cores
    ep, tp = lax.axis_index("ep"), lax.axis_index("tp")
    mirror = senders - 2

    def across(x, shift):
        return lax.ppermute(x, "ep", [(i, i ^ shift) for i in range(senders)])

    def swap(x):
        return lax.ppermute(x, "tp", [(i, cores - 1 - i) for i in range(cores)])

    values = tokens.astype(jnp.float32)
    scale = lax.rsqrt(jnp.mean(values * values, axis=-1, keepdims=True) + epsilon)
    mine = lax.dynamic_slice_in_dim(tokens, tp * half, half, 1).astype(jnp.float32)
    gain = lax.dynamic_slice_in_dim(norm_gain, tp * half, half, 0)
    normed = (mine * scale * gain).astype(jnp.bfloat16)

    table = jnp.sum(
        jnp.where(
            picks[:, :, None] == jnp.arange(group_experts, dtype=jnp.int32), gates[:, :, None], 0.0
        ),
        axis=1,
    )
    high = lax.reduce_precision(table, 8, 7)
    extra = -(2 * group_experts) % LANES
    payload = jnp.concatenate(
        [
            normed,
            high.astype(jnp.bfloat16),
            (table - high).astype(jnp.bfloat16),
            jnp.zeros((tok_rows, extra), jnp.bfloat16),
        ],
        axis=1,
    )

    order = jnp.arange(tok_rows, dtype=jnp.int32)
    same = (groups[:, None] == groups[None, :]) & (order[None, :] < order[:, None])
    position = jnp.sum(same.astype(jnp.int32), axis=1)
    target = jnp.where(groups == ep // team, 0, rows) + position
    place = (jnp.arange(GROUPS * rows, dtype=jnp.int32)[:, None] == target[None, :]).astype(
        jnp.bfloat16
    )
    packed = jnp.dot(place, payload, preferred_element_type=jnp.float32).astype(jnp.bfloat16)

    near, far = packed[:rows], packed[rows:]
    got = across(far, mirror)
    near_all = jnp.concatenate([near] + [across(near, s) for s in range(1, team)], axis=0)
    near_other = swap(near_all[:, :half])
    got_all = jnp.concatenate([got] + [across(got, s) for s in range(1, team)], axis=0)
    got_other = swap(got_all[:, :half])
    all_rows = jnp.concatenate([near_all, got_all], axis=0)
    own = all_rows[:, :half]
    other = jnp.concatenate([near_other, got_other], axis=0)
    x = jnp.concatenate(
        [jnp.where(tp == 0, own, other), jnp.where(tp == 0, other, own)], axis=1
    )
    weights = all_rows[:, half : half + 2 * group_experts].astype(jnp.float32)
    weights = weights[:, :group_experts] + weights[:, group_experts:]
    first = (ep % team) * local
    weights = lax.dynamic_slice_in_dim(weights, first, local, 1)

    hidden = []
    for j in range(local):
        g = jnp.dot(x, w_gate[j], preferred_element_type=jnp.float32)
        u = jnp.dot(x, w_up[j], preferred_element_type=jnp.float32)
        hidden.append((jax.nn.silu(g) * u * weights[:, j : j + 1]).astype(jnp.bfloat16))
    hidden = jnp.concatenate(hidden, axis=1)
    y = jnp.dot(
        hidden, w_down.reshape(hidden.shape[1], width), preferred_element_type=jnp.float32
    )
    low, high = y[:, :half], y[:, half:]
    keep = jnp.where(tp == 0, low, high)
    send = jnp.where(tp == 0, high, low).astype(jnp.bfloat16)
    part = (keep + swap(send).astype(jnp.float32)).astype(jnp.bfloat16)

    def piece(b, s):
        at = (b * team + s) * rows
        return part[at : at + rows]

    def collect(b):
        total = piece(b, 0).astype(jnp.float32)
        for s in range(1, team):
            total = total + across(piece(b, s), s).astype(jnp.float32)
        return total.astype(jnp.bfloat16)

    far = across(collect(1), mirror)
    near = collect(0)
    out = lax.dot_general(
        place,
        jnp.concatenate([near, far], axis=0),
        (((0,), (0,)), ((), ())),
        preferred_element_type=jnp.float32,
    )
    return out.astype(jnp.bfloat16)


def solution(mesh):
    in_specs = (
        P(("grp", "ep"), None),
        P(),
        P(("grp", "ep")),
        P(("grp", "ep"), None),
        P(("grp", "ep"), None),
        P("ep", None, "tp"),
        P("ep", None, "tp"),
        P("ep", "tp", None),
    )
    out_specs = P(("grp", "ep"), "tp")
    return jax.shard_map(
        on_device, mesh=mesh, in_specs=in_specs, out_specs=out_specs, check_vma=False
    )
```

```python
import jax
import jax.numpy as jnp
from jax import lax
from jax.experimental import pallas as pl
from jax.sharding import PartitionSpec as P


GROUPS = 2
LANES = 128
SUBLANES = 8

epsilon = 1e-06


def on_device(tokens, norm_gain, groups, picks, gates, w_gate, w_up, w_down):
    tok_rows, width = tokens.shape
    top = picks.shape[1]
    local = w_gate.shape[0]
    senders = lax.axis_size("ep")
    cores = lax.axis_size("tp")
    group_experts = senders * local // GROUPS
    capacity = tok_rows * top // group_experts
    rows = max(capacity, tok_rows - capacity)
    team = senders // GROUPS
    half = width // cores
    ep, tp = lax.axis_index("ep"), lax.axis_index("tp")
    mirror = senders // GROUPS * (GROUPS - 1)

    def across(x, shift):
        return lax.ppermute(x, "ep", [(i, i ^ shift) for i in range(senders)])

    def swap(x):
        return lax.ppermute(x, "tp", [(i, cores - 1 - i) for i in range(cores)])

    near, far, place = pack(
        tokens, norm_gain, groups, picks, gates, rows, team, half, group_experts
    )
    shifts = range(team - 1, 0, -1)

    def gates_of(piece):
        pair = piece[:, half : half + 2 * group_experts].astype(jnp.float32)
        return pair[:, :group_experts] + pair[:, group_experts:]

    got = across(far, mirror)
    last_got = lax.optimization_barrier(gates_of(got))
    last_near = gates_of(near)
    near = [across(near, s) for s in shifts] + [near]
    got = [across(got, s) for s in shifts] + [got]

    def expert_rows(pieces, last):
        own = jnp.concatenate(pieces, axis=0)
        weights = jnp.concatenate([gates_of(piece) for piece in pieces[:-1]] + [last], axis=0)
        weights = lax.dynamic_slice_in_dim(weights, (ep % team) * local, local, 1)
        own = own[:, :half]
        other = swap(own)
        x = jnp.concatenate(
            [jnp.where(tp == 0, own, other), jnp.where(tp == 0, other, own)], axis=1
        )
        return x, weights

    def run_experts(x, weights):
        hidden = []
        for j in range(local):
            g = jnp.dot(x, w_gate[j], preferred_element_type=jnp.float32)
            u = jnp.dot(x, w_up[j], preferred_element_type=jnp.float32)
            hidden.append((jax.nn.silu(g) * u * weights[:, j : j + 1]).astype(jnp.bfloat16))
        hidden = jnp.concatenate(hidden, axis=1)
        y = jnp.dot(
            hidden, w_down.reshape(hidden.shape[1], width), preferred_element_type=jnp.float32
        )
        low, high = y[:, :half], y[:, half:]
        keep = jnp.where(tp == 0, low, high)
        send = jnp.where(tp == 0, high, low).astype(jnp.bfloat16)
        return (keep + swap(send).astype(jnp.float32)).astype(jnp.bfloat16)

    def collect(part):
        pieces = [part[i * rows : (i + 1) * rows] for i in range(team)]
        total = pieces[-1].astype(jnp.float32)
        for piece, s in zip(pieces, shifts):
            total = total + across(piece, s).astype(jnp.float32)
        return total.astype(jnp.bfloat16)

    near_part = run_experts(*expert_rows(near, last_near))
    got_part = run_experts(*expert_rows(got, last_got))
    far = across(collect(got_part), mirror)
    near = collect(near_part)
    out = lax.dot_general(
        place,
        jnp.concatenate([near, far], axis=0),
        (((0,), (0,)), ((), ())),
        preferred_element_type=jnp.float32,
    )
    return out.astype(jnp.bfloat16)


def pack(tokens, norm_gain, groups, picks, gates, rows, team, half, group_experts):
    tok_rows, width = tokens.shape
    top = picks.shape[1]
    pad = -(-2 * group_experts // LANES) * LANES

    def kernel(tok_ref, gain_ref, group_ref, picks_ref, gates_ref, near_ref, far_ref, place_ref):
        my_group = lax.axis_index("ep") // team
        at = pl.multiple_of(lax.axis_index("tp") * half, LANES)
        values = tok_ref[...].astype(jnp.float32)
        scale = lax.rsqrt(jnp.mean(values * values, axis=-1, keepdims=True) + epsilon)
        mine = tok_ref[:, pl.ds(at, half)].astype(jnp.float32)
        normed = (mine * scale * gain_ref[:, pl.ds(at, half)]).astype(jnp.bfloat16)
        row = lax.broadcasted_iota(jnp.int32, (pad, tok_rows), 0)
        expert = jnp.where(row < group_experts, row, row - group_experts)
        table = jnp.zeros((pad, tok_rows), jnp.float32)
        for k in range(top):
            table += jnp.where(picks_ref[k : k + 1] == expert, gates_ref[k : k + 1], 0.0)
        high = table.astype(jnp.bfloat16).astype(jnp.float32)
        table = jnp.where(row < group_experts, high, table - high).astype(jnp.bfloat16)
        group = lax.broadcasted_iota(jnp.int32, (SUBLANES, tok_rows), 0)
        member = jnp.where(group_ref[...] == group, 1.0, 0.0)
        earlier = lax.broadcasted_iota(jnp.int32, (tok_rows, tok_rows), 0)
        later = lax.broadcasted_iota(jnp.int32, (tok_rows, tok_rows), 1)
        before = jnp.where(earlier < later, 1.0, 0.0).astype(jnp.bfloat16)
        ahead = jnp.dot(member.astype(jnp.bfloat16), before, preferred_element_type=jnp.float32)
        position = jnp.sum(member * ahead, axis=0, keepdims=True).astype(jnp.int32)
        target = jnp.where(group_ref[...] == my_group, 0, rows) + position
        slot = lax.broadcasted_iota(jnp.int32, (GROUPS * rows, tok_rows), 0)
        place = jnp.where(slot == target, 1.0, 0.0).astype(jnp.bfloat16)
        place_ref[...] = place
        packed = jnp.dot(place, normed, preferred_element_type=jnp.float32).astype(jnp.bfloat16)
        near_ref[:, :half] = packed[:rows]
        far_ref[:, :half] = packed[rows:]
        packed = lax.dot_general(
            place, table, (((1,), (1,)), ((), ())), preferred_element_type=jnp.float32
        ).astype(jnp.bfloat16)
        near_ref[:, half:] = packed[:rows]
        far_ref[:, half:] = packed[rows:]

    block = jax.ShapeDtypeStruct((rows, half + pad), jnp.bfloat16)
    return pl.pallas_call(
        kernel,
        out_shape=(block, block, jax.ShapeDtypeStruct((GROUPS * rows, tok_rows), jnp.bfloat16)),
    )(
        tokens,
        norm_gain.reshape(1, width),
        groups.reshape(1, tok_rows),
        picks.T,
        gates.T,
    )


def solution(mesh):
    in_specs = (
        P(("grp", "ep"), None),
        P(),
        P(("grp", "ep")),
        P(("grp", "ep"), None),
        P(("grp", "ep"), None),
        P("ep", None, "tp"),
        P("ep", None, "tp"),
        P("ep", "tp", None),
    )
    out_specs = P(("grp", "ep"), "tp")
    return jax.shard_map(
        on_device, mesh=mesh, in_specs=in_specs, out_specs=out_specs, check_vma=False
    )
```

```python
import jax
import jax.numpy as jnp
from jax import lax
from jax.experimental import pallas as pl
from jax.sharding import PartitionSpec as P


GROUPS = 2
LANES = 128
SUBLANES = 8

epsilon = 1e-06


def on_device(tokens, norm_gain, groups, picks, gates, w_gate, w_up, w_down):
    tok_rows, width = tokens.shape
    top = picks.shape[1]
    local = w_gate.shape[0]
    senders = lax.axis_size("ep")
    cores = lax.axis_size("tp")
    group_experts = senders * local // GROUPS
    capacity = tok_rows * top // group_experts
    rows = max(capacity, tok_rows - capacity)
    team = senders // GROUPS
    half = width // cores
    ep, tp = lax.axis_index("ep"), lax.axis_index("tp")
    mirror = senders // GROUPS * (GROUPS - 1)

    def across(x, shift):
        return lax.ppermute(x, "ep", [(i, i ^ shift) for i in range(senders)])

    def swap(x):
        return lax.ppermute(x, "tp", [(i, cores - 1 - i) for i in range(cores)])

    near, far, place = pack(
        tokens, norm_gain, groups, picks, gates, rows, team, half, group_experts
    )
    shifts = range(1, team)
    column = jnp.arange(near.shape[1] - half, dtype=jnp.int32)[:, None]
    expert = (ep % team) * local + jnp.arange(local, dtype=jnp.int32)[None, :]
    pick_gates = ((column == expert) | (column == expert + group_experts)).astype(jnp.bfloat16)

    def gates_of(own):
        return jnp.dot(own[:, half:], pick_gates, preferred_element_type=jnp.float32)

    got = across(far, mirror)
    last_got = lax.optimization_barrier(gates_of(got))
    near = [across(near, s) for s in shifts] + [near]
    got = [across(got, s) for s in shifts] + [got]

    def expert_rows(pieces, last):
        own = jnp.concatenate(pieces, axis=0)
        if last is None:
            weights = gates_of(own)
        else:
            weights = jnp.concatenate([gates_of(own[: -last.shape[0]]), last], axis=0)
        own = own[:, :half]
        other = swap(own)
        x = jnp.concatenate(
            [jnp.where(tp == 0, own, other), jnp.where(tp == 0, other, own)], axis=1
        )
        return x, weights

    def run_experts(x, weights):
        hidden = []
        for j in range(local):
            g = jnp.dot(x, w_gate[j], preferred_element_type=jnp.float32)
            u = jnp.dot(x, w_up[j], preferred_element_type=jnp.float32)
            hidden.append((jax.nn.silu(g) * u * weights[:, j : j + 1]).astype(jnp.bfloat16))
        hidden = jnp.concatenate(hidden, axis=1)
        y = jnp.dot(
            hidden, w_down.reshape(hidden.shape[1], width), preferred_element_type=jnp.float32
        )
        low, high = y[:, :half], y[:, half:]
        keep = jnp.where(tp == 0, low, high)
        send = jnp.where(tp == 0, high, low).astype(jnp.bfloat16)
        return (keep + swap(send).astype(jnp.float32)).astype(jnp.bfloat16)

    def collect(part, own):
        pieces = [part[i * rows : (i + 1) * rows] for i in range(team)]
        sent = [across(piece, s) for piece, s in zip(pieces, shifts)]
        total = sum(piece.astype(jnp.float32) for piece in (sent + pieces[-1:] if own else sent))
        return total.astype(jnp.bfloat16)

    def in_order(part, at):
        return lax.dot_general(
            place[at], part, (((0,), (0,)), ((), ())), preferred_element_type=jnp.float32
        )

    near_part = run_experts(*expert_rows(near, None))
    got_part = run_experts(*expert_rows(got, last_got))
    far = across(collect(got_part, True), mirror)
    near = collect(near_part, False)
    own = lax.optimization_barrier(in_order(near_part[-rows:], slice(0, rows)))
    out = own + in_order(jnp.concatenate([near, far], axis=0), slice(None))
    return out.astype(jnp.bfloat16)


def pack(tokens, norm_gain, groups, picks, gates, rows, team, half, group_experts):
    tok_rows, width = tokens.shape
    top = picks.shape[1]
    pad = -(-2 * group_experts // LANES) * LANES

    def kernel(tok_ref, gain_ref, group_ref, picks_ref, gates_ref, near_ref, far_ref, place_ref):
        my_group = lax.axis_index("ep") // team
        at = pl.multiple_of(lax.axis_index("tp") * half, LANES)
        values = tok_ref[...].astype(jnp.float32)
        scale = lax.rsqrt(jnp.mean(values * values, axis=-1, keepdims=True) + epsilon)
        mine = tok_ref[:, pl.ds(at, half)].astype(jnp.float32)
        normed = (mine * scale * gain_ref[:, pl.ds(at, half)]).astype(jnp.bfloat16)
        row = lax.broadcasted_iota(jnp.int32, (pad, tok_rows), 0)
        expert = jnp.where(row < group_experts, row, row - group_experts)
        table = jnp.zeros((pad, tok_rows), jnp.float32)
        for k in range(top):
            table += jnp.where(picks_ref[k : k + 1] == expert, gates_ref[k : k + 1], 0.0)
        high = table.astype(jnp.bfloat16).astype(jnp.float32)
        table = jnp.where(row < group_experts, high, table - high).astype(jnp.bfloat16)
        group = lax.broadcasted_iota(jnp.int32, (SUBLANES, tok_rows), 0)
        member = jnp.where(group_ref[...] == group, 1.0, 0.0)
        earlier = lax.broadcasted_iota(jnp.int32, (tok_rows, tok_rows), 0)
        later = lax.broadcasted_iota(jnp.int32, (tok_rows, tok_rows), 1)
        before = jnp.where(earlier < later, 1.0, 0.0).astype(jnp.bfloat16)
        ahead = jnp.dot(member.astype(jnp.bfloat16), before, preferred_element_type=jnp.float32)
        position = jnp.sum(member * ahead, axis=0, keepdims=True).astype(jnp.int32)
        target = jnp.where(group_ref[...] == my_group, 0, rows) + position
        slot = lax.broadcasted_iota(jnp.int32, (GROUPS * rows, tok_rows), 0)
        place = jnp.where(slot == target, 1.0, 0.0).astype(jnp.bfloat16)
        place_ref[...] = place
        packed = jnp.dot(place, normed, preferred_element_type=jnp.float32).astype(jnp.bfloat16)
        near_ref[:, :half] = packed[:rows]
        far_ref[:, :half] = packed[rows:]
        packed = lax.dot_general(
            place, table, (((1,), (1,)), ((), ())), preferred_element_type=jnp.float32
        ).astype(jnp.bfloat16)
        near_ref[:, half:] = packed[:rows]
        far_ref[:, half:] = packed[rows:]

    block = jax.ShapeDtypeStruct((rows, half + pad), jnp.bfloat16)
    return pl.pallas_call(
        kernel,
        out_shape=(block, block, jax.ShapeDtypeStruct((GROUPS * rows, tok_rows), jnp.bfloat16)),
    )(
        tokens,
        norm_gain.reshape(1, width),
        groups.reshape(1, tok_rows),
        picks.T,
        gates.T,
    )


def solution(mesh):
    in_specs = (
        P(("grp", "ep"), None),
        P(),
        P(("grp", "ep")),
        P(("grp", "ep"), None),
        P(("grp", "ep"), None),
        P("ep", None, "tp"),
        P("ep", None, "tp"),
        P("ep", "tp", None),
    )
    out_specs = P(("grp", "ep"), "tp")
    return jax.shard_map(
        on_device, mesh=mesh, in_specs=in_specs, out_specs=out_specs, check_vma=False
    )
```
